32 devices in a mesh: sp: 8 (over z, x), tp: 4 (over y, core).
Axes of the slice: x: 2, y: 2, z: 4, core: 2. Of those that a mesh axis runs over, the one named last changes fastest.
Arguments:
- queries: bfloat16 [1536, 1536], P('sp', 'tp'), may hold values from -64 to 64
- latents: bfloat16 [1536, 512], P('sp'), may hold values from -6 to 6
- rope_key: bfloat16 [1536, 32], P('sp'), may hold values from -64 to 64
- w_key: bfloat16 [512, 1024], P(None, 'tp'), may hold values from -0.25 to 0.25
- w_value: bfloat16 [512, 1024], P(None, 'tp'), may hold values from -0.25 to 0.25
- w_out: bfloat16 [1024, 2048], P('tp'), may hold values from -0.59765625 to 0.59765625
- resid: bfloat16 [1536, 2048], P('sp', 'tp'), may hold values from -12 to 12
- gain_mix: float32 [2048], P('tp'), may hold values from 0.1 to 1.9
- w_gate: bfloat16 [2048, 3072], P('sp', 'tp'), may hold values from -0.125 to 0.125
- w_up: bfloat16 [2048, 3072], P('sp', 'tp'), may hold values from -0.125 to 0.125
- w_down: bfloat16 [3072, 2048], P('tp', 'sp'), may hold values from -0.41992188 to 0.41992188
- gain_out: float32 [2048], P('tp'), may hold values from 0.1 to 1.9
Outputs:
- layer_out: bfloat16 [1536, 2048], P('sp', 'tp')
The draws below stay inside these ranges and needn't reach their ends.
All inputs are finite; a program needn't handle non-finite values.
Results may differ from the reference program's by a relative error of at most 0.014.
Values may be sent and summed in bfloat16 or wider, within the bound.
No kernel may reach another device: no remote copies, remote signals or barrier semaphores. Data moves between devices by JAX's collectives and lax.ppermute only.
A program may use at most 128 MiB of HBM per device.

```python
import math
import jax
import jax.numpy as jnp
from jax import lax

D = 2048
HEADS = 16
NOPE = 64
ROPE = 32
VDIM = 64
KV_RANK = 512
FF = 3072
GRID_W = 64
TOKENS = 1536
N_TP = 4


def drawn_pair(key):
    query_seed = jax.random.fold_in(key, 11)
    rotary_seed = jax.random.fold_in(key, 12)
    width_total = HEADS * (NOPE + ROPE)
    queries = jnp.clip(jax.random.normal(query_seed, (TOKENS, width_total), jnp.float32) * 2.5, -15.0, 15.0)
    rotary = jnp.clip(jax.random.normal(rotary_seed, (TOKENS, ROPE), jnp.float32), -6.0, 6.0)
    return (queries, rotary)


def draw_queries(key, part):
    return drawn_pair(key)[0].astype(jnp.bfloat16)


def draw_rope_key(key, part):
    return drawn_pair(key)[1].astype(jnp.bfloat16)


def draw_resid(key, part):
    row_seed = jax.random.fold_in(key, 21)
    value_seed = jax.random.fold_in(key, 22)
    column_scale = 0.6 * 10.0 ** (jnp.arange(D, dtype=jnp.float32) / (D - 1) - 0.5)
    row_scale = 10.0 ** jax.random.uniform(row_seed, (TOKENS, 1), jnp.float32, -0.5, 0.5)
    values_out = jax.random.normal(value_seed, (TOKENS, D), jnp.float32) * row_scale * column_scale
    return jnp.clip(values_out, -12.0, 12.0).astype(jnp.bfloat16)


def steps_of(key, shape, cuts, low, largest):
    gain, own = 1.0, jax.random.fold_in(key, 6)
    for axis_at, shards_of in cuts:
        draws = jnp.exp(jax.random.uniform(jax.random.fold_in(own, axis_at), (shards_of,), jnp.float32, low / len(cuts), largest / len(cuts)))
        gain = gain * jnp.repeat(draws, shape[axis_at] // shards_of).reshape([-1 if axis == axis_at else 1 for axis in range(len(shape))])
    return gain


def gaussian(stream_key, shape, spread, limit, pieces=(), kind=jnp.bfloat16):
    result = jax.random.normal(stream_key, shape, jnp.float32) * spread
    if len(pieces) > 0:
        result = steps_of(stream_key, shape, pieces, -0.22, 0.18) * result
    return jnp.clip(result, min=-limit, max=limit).astype(kind)


def setup_inputs(seed: int = 0) -> dict:
    keys = jax.random.split(jax.random.key(seed), 13)
    queries = draw_queries(jax.random.fold_in(keys[12], 71), 0)
    latents = gaussian(keys[1], (TOKENS, KV_RANK), 1.0, 6.0, ((0, 8),))
    rope_key = draw_rope_key(jax.random.fold_in(keys[12], 71), 0)
    w_key = gaussian(keys[3], (KV_RANK, HEADS * NOPE), KV_RANK ** -0.5, 0.25, ((1, 4),))
    w_value = gaussian(keys[4], (KV_RANK, HEADS * VDIM), KV_RANK ** -0.5, 0.25, ((1, 4),))
    w_out = gaussian(keys[5], (HEADS * VDIM, D), 0.1, 0.59765625, ((0, 4),))
    resid = draw_resid(jax.random.fold_in(keys[12], 71), 0)
    gain_mix = jnp.clip(1.0 + 0.18 * jax.random.normal(keys[7], (D,), jnp.float32), 0.1, 1.9)
    w_gate = gaussian(keys[8], (D, FF), D ** -0.5, 0.125, ((0, 8), (1, 4)))
    w_up = gaussian(keys[9], (D, FF), D ** -0.5, 0.125, ((0, 8), (1, 4)))
    w_down = gaussian(keys[10], (FF, D), 0.07, 0.41992188, ((0, 4), (1, 8)))
    gain_out = jnp.clip(1.0 + 0.18 * jax.random.normal(keys[11], (D,), jnp.float32), 0.1, 1.9)
    return {"queries": queries, "latents": latents, "rope_key": rope_key, "w_key": w_key, "w_value": w_value, "w_out": w_out, "resid": resid, "gain_mix": gain_mix, "w_gate": w_gate, "w_up": w_up, "w_down": w_down, "gain_out": gain_out}


ROTARY_BASE = 10000.0
NORM_EPSILON = 1e-06
DEEP_ALPHA = 8.0 ** 0.25
HALF_STEP = 0.5

def rotary_tables(positions, rotary_width, grid_width):
    grid_rows = (positions // grid_width).astype(jnp.float32)
    grid_cols = (positions % grid_width).astype(jnp.float32)
    freq_count = rotary_width // 4
    inverse = ROTARY_BASE ** (-jnp.arange(freq_count, dtype=jnp.float32) / freq_count)
    angle_table = jnp.concatenate([grid_rows[:, None] * inverse, grid_cols[:, None] * inverse], axis=-1)
    return (jnp.cos(angle_table), jnp.sin(angle_table))

def rotate(vectors, cosine, sine):
    half_width = vectors.shape[-1] // 2
    leading = vectors[..., :half_width].astype(jnp.float32)
    trailing = vectors[..., half_width:].astype(jnp.float32)
    return jnp.concatenate([leading * cosine - trailing * sine, leading * sine + trailing * cosine], axis=-1).astype(jnp.bfloat16)

def widened(tensor):
    return lax.optimization_barrier(tensor.astype(jnp.bfloat16)).astype(jnp.float32)

def layer_norm(rows_in, gain_row):
    row_mean = lax.optimization_barrier(jnp.mean(rows_in, axis=1, keepdims=True))
    variance = lax.optimization_barrier(jnp.mean(rows_in * rows_in, axis=1, keepdims=True)) - row_mean * row_mean
    return ((rows_in - row_mean) * lax.rsqrt(variance + NORM_EPSILON) * gain_row.astype(jnp.float32)).astype(jnp.bfloat16)

def group_sum(left, right, group_width):
    total_sum = jnp.zeros((left.shape[0], right.shape[1]), jnp.float32)
    for group_index in range(N_TP):
        lower = group_index * group_width
        partial_term = jnp.dot(left[:, lower:lower + group_width], right[lower:lower + group_width], preferred_element_type=jnp.float32)
        total_sum = total_sum + widened(partial_term)
    return total_sum

def reference(queries, latents, rope_key, w_key, w_value, w_out, resid, gain_mix, w_gate, w_up, w_down, gain_out):
    positions = jnp.arange(TOKENS, dtype=jnp.int32)
    cosine, sine = rotary_tables(positions, ROPE, GRID_W)
    key_rot = lax.optimization_barrier(rotate(rope_key, cosine, sine)).astype(jnp.float32)
    shaped = queries.reshape(TOKENS, HEADS, NOPE + ROPE)
    q_nope = shaped[:, :, :NOPE]
    q_rot = rotate(shaped[:, :, NOPE:], cosine[:, None, :], sine[:, None, :])
    key_nope = widened(jnp.dot(latents, w_key, preferred_element_type=jnp.float32)).reshape(TOKENS, HEADS, NOPE)
    head_values = widened(jnp.dot(latents, w_value, preferred_element_type=jnp.float32)).reshape(TOKENS, HEADS, VDIM)
    block_rows = math.gcd(TOKENS, 512)
    score_scale = (NOPE + ROPE) ** (-0.5)

    def attend(block_index):
        first_row = (block_index * block_rows).astype(jnp.int32)
        query_nope = lax.dynamic_slice_in_dim(q_nope, first_row, block_rows, 0).astype(jnp.float32)
        query_rope = lax.dynamic_slice_in_dim(q_rot, first_row, block_rows, 0).astype(jnp.float32)
        scores = jnp.einsum('qhd,khd->hqk', query_nope, key_nope) + jnp.einsum('qhd,kd->hqk', query_rope, key_rot)
        scores = scores * score_scale
        row_max = lax.optimization_barrier(jnp.max(scores, axis=-1, keepdims=True))
        weights = jnp.exp(scores - row_max)
        totals = lax.optimization_barrier(jnp.sum(weights, axis=-1))
        prob_weights = widened(weights)
        heads_block = jnp.einsum('hqk,khd->qhd', prob_weights, head_values) / jnp.transpose(totals)[:, :, None]
        return heads_block.astype(jnp.bfloat16).reshape(block_rows, HEADS * VDIM)
    heads_out = lax.map(attend, jnp.arange(TOKENS // block_rows, dtype=jnp.int32)).reshape(TOKENS, HEADS * VDIM)
    attn_sum = group_sum(heads_out, w_out, HEADS * VDIM // N_TP)
    mixed_in = DEEP_ALPHA * resid.astype(jnp.float32) + attn_sum
    hidden_in = layer_norm(mixed_in, gain_mix)
    gate_sum = jnp.dot(hidden_in, w_gate, preferred_element_type=jnp.float32)
    up_sum = jnp.dot(hidden_in, w_up, preferred_element_type=jnp.float32)
    hidden = (jax.nn.silu(gate_sum) * up_sum).astype(jnp.bfloat16)
    mixer_sum = group_sum(hidden, w_down, FF // N_TP)
    return layer_norm(DEEP_ALPHA * hidden_in.astype(jnp.float32) + HALF_STEP * mixer_sum, gain_out)
```

```python
import functools

import jax
import jax.numpy as jnp
from jax import lax
from jax.experimental import pallas as pl
from jax.experimental.pallas import tpu as pltpu
from jax.sharding import PartitionSpec as P

NOPE = 64
ROPE = 32
VDIM = 64
GRID_W = 64


ROTARY_BASE = 10000.0
NORM_EPSILON = 1e-06
DEEP_ALPHA = 8.0**0.25
HALF_STEP = 0.5


def rotary_tables(positions, rotary_width, grid_width):
    grid_rows = (positions // grid_width).astype(jnp.float32)
    grid_cols = (positions % grid_width).astype(jnp.float32)
    freq_count = rotary_width // 4
    inverse = ROTARY_BASE ** (-jnp.arange(freq_count, dtype=jnp.float32) / freq_count)
    angle_table = jnp.concatenate(
        [grid_rows[:, None] * inverse, grid_cols[:, None] * inverse], axis=-1
    )
    return (jnp.cos(angle_table), jnp.sin(angle_table))


def rotate(vectors, cosine, sine):
    half_width = vectors.shape[-1] // 2
    leading = vectors[..., :half_width].astype(jnp.float32)
    trailing = vectors[..., half_width:].astype(jnp.float32)
    return jnp.concatenate(
        [leading * cosine - trailing * sine, leading * sine + trailing * cosine], axis=-1
    ).astype(jnp.bfloat16)


def attend_block(state, key_block, query_pair):
    maxima, totals, running = state
    key_nope, value_rows, key_rope = key_block
    q_nope, q_rope = query_pair
    head_count = q_nope.shape[1]
    rows_here = key_nope.shape[0]
    key_nope = key_nope.reshape(rows_here, head_count, -1)
    value_rows = value_rows.reshape(rows_here, head_count, -1)
    score_scale = (q_nope.shape[2] + q_rope.shape[2]) ** (-0.5)
    scores = jnp.einsum("qhd,khd->hqk", q_nope, key_nope, preferred_element_type=jnp.float32)
    scores = (
        scores + jnp.einsum("qhd,kd->hqk", q_rope, key_rope, preferred_element_type=jnp.float32)
    ) * score_scale
    new_max = jnp.maximum(maxima, jnp.max(scores, axis=-1))
    weights = jnp.exp(scores - new_max[:, :, None])
    factor = jnp.exp(maxima - new_max)
    totals = totals * factor + jnp.sum(weights, axis=-1)
    update = jnp.einsum(
        "hqk,khd->qhd", weights.astype(jnp.bfloat16), value_rows, preferred_element_type=jnp.float32
    )
    running = running * jnp.transpose(factor)[:, :, None] + update
    return (new_max, totals, running)


def block_length(length):
    block_rows = length
    while block_rows > 2048 and block_rows % 2 == 0:
        block_rows = block_rows // 2
    return block_rows


def fold_keys(state, pieces, query_pair):
    length = pieces[0].shape[0]
    block_rows = block_length(length)
    if block_rows == length:
        return attend_block(state, pieces, query_pair)
    stacked = tuple(
        (member.reshape(length // block_rows, block_rows, member.shape[1]) for member in pieces)
    )

    def one_block(partial_value, key_block):
        return (attend_block(partial_value, key_block, query_pair), None)

    state, unused = lax.scan(one_block, state, stacked)
    return state


def split_norm(rows_in, gain_row):
    width_total = rows_in.shape[1] * lax.axis_size("tp")
    row_sums, squares = lax.psum(
        (jnp.sum(rows_in, axis=1), jnp.sum(rows_in * rows_in, axis=1)), "tp"
    )
    row_mean = row_sums / width_total
    variance = squares / width_total - row_mean * row_mean
    return (
        (rows_in - row_mean[:, None]) * lax.rsqrt(variance + NORM_EPSILON)[:, None] * gain_row
    ).astype(jnp.bfloat16)


def local(
    queries,
    latents,
    rope_key,
    w_key,
    w_value,
    w_out,
    resid,
    gain_mix,
    w_gate,
    w_up,
    w_down,
    gain_out,
):
    local_rows = queries.shape[0]
    head_count = w_key.shape[1] // NOPE
    offset = lax.axis_index("sp") * local_rows
    positions = offset + jnp.arange(local_rows, dtype=jnp.int32)
    cosine, sine = rotary_tables(positions, ROPE, GRID_W)
    key_rot = rotate(rope_key, cosine, sine)
    shaped = queries.reshape(local_rows, head_count, NOPE + ROPE)
    q_nope = shaped[:, :, :NOPE]
    q_rot = rotate(shaped[:, :, NOPE:], cosine[:, None, :], sine[:, None, :])
    query_pair = (q_nope, q_rot)
    start_state = (
        jnp.full((head_count, local_rows), -jnp.inf, jnp.float32),
        jnp.zeros((head_count, local_rows), jnp.float32),
        jnp.zeros((local_rows, head_count, VDIM), jnp.float32),
    )
    quarter = local_rows // lax.axis_size("tp")
    first_row = lax.axis_index("tp") * quarter
    latent_part = lax.dynamic_slice_in_dim(latents, first_row, quarter, 0)
    rotary_part = lax.dynamic_slice_in_dim(key_rot, first_row, quarter, 0)
    latent_all, rotary_all = (
        lax.all_gather(latent_part, "sp", axis=0, tiled=True),
        lax.all_gather(rotary_part, "sp", axis=0, tiled=True),
    )
    pieces = (
        lax.all_gather(latent_all, "tp", axis=0, tiled=True),
        lax.all_gather(rotary_all, "tp", axis=0, tiled=True),
    )
    key_nope = jnp.dot(pieces[0], w_key, preferred_element_type=jnp.float32).astype(jnp.bfloat16)
    value_rows = jnp.dot(pieces[0], w_value, preferred_element_type=jnp.float32).astype(
        jnp.bfloat16
    )
    state = fold_keys(start_state, (key_nope, value_rows, pieces[1]), query_pair)
    maxima, totals, running = state
    heads_out = (
        (running / jnp.transpose(totals)[:, :, None])
        .reshape(local_rows, head_count * VDIM)
        .astype(jnp.bfloat16)
    )
    projected = jnp.dot(heads_out, w_out, preferred_element_type=jnp.float32)
    attn_cols = lax.psum_scatter(
        projected.astype(jnp.bfloat16), "tp", scatter_dimension=1, tiled=True
    ).astype(jnp.float32)
    hidden_in = split_norm(DEEP_ALPHA * resid.astype(jnp.float32) + attn_cols, gain_mix)
    whole_rows = lax.all_gather(hidden_in, "tp", axis=1, tiled=True)
    pieces = (
        lax.all_gather(w_gate, "sp", axis=0, tiled=True),
        lax.all_gather(w_up, "sp", axis=0, tiled=True),
    )
    gate_sum = jnp.dot(whole_rows, pieces[0], preferred_element_type=jnp.float32)
    up_sum = jnp.dot(whole_rows, pieces[1], preferred_element_type=jnp.float32)
    hidden = (jax.nn.silu(gate_sum) * up_sum).astype(jnp.bfloat16)
    down_terms = jnp.dot(
        hidden, lax.all_gather(w_down, "sp", axis=1, tiled=True), preferred_element_type=jnp.float32
    )
    mixer_cols = lax.psum_scatter(
        down_terms.astype(jnp.bfloat16), "tp", scatter_dimension=1, tiled=True
    ).astype(jnp.float32)
    return split_norm(DEEP_ALPHA * hidden_in.astype(jnp.float32) + HALF_STEP * mixer_cols, gain_out)


RING = 4
PAIR = 2
LANES = 128
BOTH = ("sp", "tp")
VMEM = pl.BlockSpec(memory_space=pltpu.VMEM)
HBM = pl.BlockSpec(memory_space=pl.ANY)
PARAMS = pltpu.CompilerParams(vmem_limit_bytes=56 * 1024 * 1024)


def fits_plan(mesh):
    return mesh.shape["sp"] == RING * PAIR and mesh.shape["tp"] == PAIR * PAIR


def move(array, where):
    pairs = []
    for z in range(RING):
        for x in range(PAIR):
            for y in range(PAIR):
                for c in range(PAIR):
                    to_z, to_x, to_y, to_c = where(z, x, y, c)
                    here = (z * PAIR + x) * PAIR * PAIR + y * PAIR + c
                    there = (to_z * PAIR + to_x) * PAIR * PAIR + to_y * PAIR + to_c
                    pairs.append((here, there))
    return lax.ppermute(array, BOTH, pairs)


def flip(array, dz=0, dx=0, dy=0, dc=0):
    return move(array, lambda z, x, y, c: (z ^ dz, x ^ dx, y ^ dy, c ^ dc))


def partner(array):
    return flip(array, dc=1)


def exchange_halves(array):
    return move(array, lambda z, x, y, c: (z, c, y, x))


ROUNDS = ((0, 0), (0, 1), (1, 0), (1, 1))


def spread(array, dy, k):
    return move(array, lambda z, x, y, c: (z, c ^ k, y ^ dy, x))


def collect(array, dy, k):
    return move(array, lambda z, x, y, c: (z, c, y ^ dy, x ^ k))


def coordinates():
    sp = lax.axis_index("sp")
    tp = lax.axis_index("tp")
    return (sp // PAIR, sp % PAIR, tp // PAIR, tp % PAIR)


def other(bit):
    return 1 - bit


def round_block(dy, k, x, y):
    row = other(y) if dy else y
    column = other(x) if k else x
    return row * PAIR + column


def attention_kernel(scale, n_blocks, *refs):
    q_ref = refs[0]
    blocks = refs[1 : 1 + n_blocks]
    wk_ref, wv_ref, out_ref, k_scr, v_scr = refs[1 + n_blocks :]
    rank = wk_ref.shape[0]
    tiles = wk_ref.shape[1] // LANES
    offset = 0
    for ref in blocks:
        rows = ref.shape[0]
        lat = ref[:, :rank]
        keys = jnp.dot(lat, wk_ref[...], preferred_element_type=jnp.float32).astype(jnp.bfloat16)
        values = jnp.dot(lat, wv_ref[...], preferred_element_type=jnp.float32).astype(jnp.bfloat16)
        for tile in range(tiles):
            k_scr[tile, offset : offset + rows, :LANES] = keys[:, tile * LANES : (tile + 1) * LANES]
            k_scr[tile, offset : offset + rows, LANES:] = ref[:, rank:]
        v_scr[offset : offset + rows, :] = values
        offset += rows
    heads_per_tile = LANES // NOPE
    for tile in range(tiles):
        merged = None
        for part in range(heads_per_tile):
            scores = lax.dot_general(
                q_ref[tile * heads_per_tile + part],
                k_scr[tile],
                (((1,), (1,)), ((), ())),
                preferred_element_type=jnp.float32,
            )
            top = jnp.max(scores, axis=-1, keepdims=True)
            weights = jnp.exp((scores - top) * scale)
            total = jnp.sum(weights, axis=-1, keepdims=True)
            update = jnp.dot(
                weights.astype(jnp.bfloat16),
                v_scr[:, tile * LANES : (tile + 1) * LANES],
                preferred_element_type=jnp.float32,
            )
            update = update / total
            lane = lax.broadcasted_iota(jnp.int32, update.shape, 1)
            mine = (lane >= part * NOPE) & (lane < (part + 1) * NOPE)
            merged = update if merged is None else jnp.where(mine, update, merged)
        out_ref[:, tile * LANES : (tile + 1) * LANES] = merged.astype(jnp.bfloat16)


def attend(q_tiles, blocks, w_key, w_value):
    keys = sum(block.shape[0] for block in blocks)
    tiles = w_key.shape[1] // LANES
    rows = q_tiles.shape[1]
    return pl.pallas_call(
        functools.partial(attention_kernel, (NOPE + ROPE) ** (-0.5), len(blocks)),
        out_shape=jax.ShapeDtypeStruct((rows, w_value.shape[1]), jnp.bfloat16),
        in_specs=[VMEM] * (len(blocks) + 3),
        out_specs=VMEM,
        scratch_shapes=[
            pltpu.VMEM((tiles, keys, 2 * LANES), jnp.bfloat16),
            pltpu.VMEM((keys, w_value.shape[1]), jnp.bfloat16),
        ],
        compiler_params=PARAMS,
        name="attend",
    )(q_tiles, *blocks, w_key, w_value)


def mix_kernel(*refs):
    heads = refs[0:4]
    w_refs = refs[4:8]
    resid_refs = refs[8:12]
    hid_ref, own_ref, other_ref, w_scr, res_scr, gain_scr, sems = refs[12:]
    z, x, y, c = coordinates()
    turned = (x + c) % PAIR
    copies = []
    for j in range(4):
        slot = j + turned * (1 - 2 * (j % PAIR))
        copy = pltpu.make_async_copy(w_refs[j], w_scr.at[slot], sems.at[j])
        copy.start()
        copies.append(copy)
    rows = hid_ref.shape[0]
    width = own_ref.shape[1]
    for j, (dy, k) in enumerate(ROUNDS):
        columns = pl.ds(pl.multiple_of(round_block(dy, k, x, y) * width, width), width)
        res_scr[:, columns] = DEEP_ALPHA * resid_refs[j][:rows, :].astype(jnp.float32)
        gains = resid_refs[j][rows:, :].astype(jnp.float32)
        gain_scr[:, columns] = gains[0:1] + gains[1:2] + gains[2:3]
    for copy in copies:
        copy.wait()
    mixed = res_scr[...]
    for j in range(4):
        mixed = mixed + jnp.dot(heads[j][...], w_scr[j], preferred_element_type=jnp.float32)
    mean = jnp.mean(mixed, axis=1, keepdims=True)
    variance = jnp.mean(mixed * mixed, axis=1, keepdims=True) - mean * mean
    res_scr[...] = (mixed - mean) * lax.rsqrt(variance + NORM_EPSILON) * gain_scr[...]
    hid_ref[...] = res_scr[...].astype(jnp.bfloat16)
    mine = y * PAIR + c
    theirs = y * PAIR + other(c)
    own_ref[...] = res_scr[:, pl.ds(pl.multiple_of(mine * width, width), width)].astype(jnp.bfloat16)
    other_ref[...] = res_scr[:, pl.ds(pl.multiple_of(theirs * width, width), width)].astype(
        jnp.bfloat16
    )


def mix(heads, w_pieces, resid_pieces):
    rows = heads[0].shape[0]
    depth, width_total = w_pieces[0].shape
    width = resid_pieces[0].shape[1]
    block = jax.ShapeDtypeStruct((rows, width), jnp.bfloat16)
    return pl.pallas_call(
        mix_kernel,
        out_shape=(jax.ShapeDtypeStruct((rows, width_total), jnp.bfloat16), block, block),
        in_specs=[VMEM] * 4 + [HBM] * 4 + [VMEM] * 4,
        out_specs=(VMEM,) * 3,
        scratch_shapes=[
            pltpu.VMEM((4, depth, width_total), jnp.bfloat16),
            pltpu.VMEM((rows, width_total), jnp.float32),
            pltpu.VMEM((1, width_total), jnp.float32),
            pltpu.SemaphoreType.DMA((4,)),
        ],
        compiler_params=PARAMS,
        name="mix",
    )(*heads, *w_pieces, *resid_pieces)


def feed_kernel(*refs):
    hid_ref = refs[0]
    pieces = refs[1:11]
    outs = refs[11:15]
    g_scr, u_scr, d_scr, sems = refs[15:]
    z, x, y, c = coordinates()
    depth = d_scr.shape[2]
    units = g_scr.shape[1]
    cuts = units // depth
    near = z + 1 - 2 * (z % 2)
    far = RING - 1 - z
    across = (z + 2) % RING
    half = pieces[3].shape[0]
    copies = []

    def fetch(source, target):
        copy = pltpu.make_async_copy(source, target, sems.at[len(copies)])
        copy.start()
        copies.append(copy)

    for side in range(2):
        part = c if side == 0 else other(c)
        group = pieces[side * 5 : side * 5 + 5]
        for ref, home in zip(group[:3], (z, near, far)):
            block = home * PAIR + part
            start = pl.ds(pl.multiple_of(block * depth, depth), depth)
            fetch(ref.at[pl.ds(0, depth)], g_scr.at[start])
            fetch(ref.at[pl.ds(depth, depth)], u_scr.at[start])
            for j in range(cuts):
                fetch(
                    ref.at[pl.ds(2 * depth, depth), pl.ds(j * depth, depth)],
                    d_scr.at[block, pl.ds(j * depth, depth)],
                )
        block = across * PAIR + part
        low, high = group[3:]
        rest = half - depth
        base = pl.multiple_of(block * depth, depth)
        fetch(low.at[pl.ds(0, depth)], g_scr.at[pl.ds(base, depth)])
        fetch(low.at[pl.ds(depth, rest)], u_scr.at[pl.ds(base, rest)])
        fetch(high.at[pl.ds(0, depth - rest)], u_scr.at[pl.ds(base + rest, depth - rest)])
        for j in range(cuts):
            fetch(
                high.at[pl.ds(depth - rest, depth), pl.ds(j * depth, depth)],
                d_scr.at[block, pl.ds(j * depth, depth)],
            )
    for copy in copies:
        copy.wait()
    hid = hid_ref[...]
    gate = jnp.dot(hid, g_scr[...], preferred_element_type=jnp.float32)
    up = jnp.dot(hid, u_scr[...], preferred_element_type=jnp.float32)
    act = (gate / (1.0 + jnp.exp(-gate)) * up).astype(jnp.bfloat16)
    for j, (dy, k) in enumerate(ROUNDS):
        block = round_block(dy, k, x, y)
        for part in range(PAIR):
            outs[j][:, part * depth : (part + 1) * depth] = jnp.dot(
                act, d_scr[block * PAIR + part], preferred_element_type=jnp.float32
            ).astype(jnp.bfloat16)


def feed(hidden_in, pieces, depth):
    rows, width_total = hidden_in.shape
    units = pieces[0].shape[1]
    block = jax.ShapeDtypeStruct((rows, PAIR * depth), jnp.bfloat16)
    n_blocks = RING * PAIR
    return pl.pallas_call(
        feed_kernel,
        out_shape=(block,) * 4,
        in_specs=[VMEM] + [HBM] * 10,
        out_specs=(VMEM,) * 4,
        scratch_shapes=[
            pltpu.VMEM((width_total, units), jnp.bfloat16),
            pltpu.VMEM((width_total, units), jnp.bfloat16),
            pltpu.VMEM((n_blocks, units, depth), jnp.bfloat16),
            pltpu.SemaphoreType.DMA((64,)),
        ],
        compiler_params=PARAMS,
        name="feed",
    )(hidden_in, *pieces)


def sum_kernel(a_ref, b_ref, c_ref, d_ref, own_ref, got_ref, pre_ref, stat_ref):
    z, x, y, c = coordinates()
    total = (
        a_ref[...].astype(jnp.float32)
        + b_ref[...].astype(jnp.float32)
        + c_ref[...].astype(jnp.float32)
        + d_ref[...].astype(jnp.float32)
    )
    same = (jnp.zeros(own_ref.shape, jnp.int32) + x) == c
    skip = jnp.where(same, own_ref[...].astype(jnp.float32), got_ref[...].astype(jnp.float32))
    pre = DEEP_ALPHA * skip + HALF_STEP * total
    pre_ref[...] = pre
    rows = pre.shape[0]
    lane = lax.broadcasted_iota(jnp.int32, (rows, LANES), 1)
    sums = jnp.sum(pre, axis=1, keepdims=True)
    squares = jnp.sum(pre * pre, axis=1, keepdims=True)
    table = jnp.where(lane == 0, sums, jnp.where(lane == 1, squares, 0.0))
    stat_ref[...] = jnp.transpose(table)[: stat_ref.shape[0], :]


def add_up(parts, own, got):
    rows, width = own.shape
    return pl.pallas_call(
        sum_kernel,
        out_shape=(
            jax.ShapeDtypeStruct((rows, width), jnp.float32),
            jax.ShapeDtypeStruct((8, rows), jnp.float32),
        ),
        in_specs=[VMEM] * 6,
        out_specs=(VMEM,) * 2,
        compiler_params=PARAMS,
        name="add_up",
    )(*parts, own, got)


def norm_kernel(width_total, pre_ref, a_ref, b_ref, c_ref, d_ref, gain_ref, out_ref):
    stats = a_ref[...] + b_ref[...] + c_ref[...] + d_ref[...]
    tall = jnp.concatenate(
        [stats, jnp.zeros((LANES - stats.shape[0], stats.shape[1]), jnp.float32)], axis=0
    )
    table = jnp.transpose(tall)
    mean = table[:, 0:1] / width_total
    variance = table[:, 1:2] / width_total - mean * mean
    out_ref[...] = (
        (pre_ref[...] - mean) * lax.rsqrt(variance + NORM_EPSILON) * gain_ref[...]
    ).astype(jnp.bfloat16)


def finish(pre, stats, gain):
    return pl.pallas_call(
        functools.partial(norm_kernel, pre.shape[1] * PAIR * PAIR),
        out_shape=jax.ShapeDtypeStruct(pre.shape, jnp.bfloat16),
        in_specs=[VMEM] * 6,
        out_specs=VMEM,
        compiler_params=PARAMS,
        name="finish",
    )(pre, *stats, gain.reshape(1, -1))


def three_terms(gain):
    first = lax.reduce_precision(gain, 8, 7)
    left = gain - first
    second = lax.reduce_precision(left, 8, 7)
    third = left - second
    return jnp.stack([first, second, third]).astype(jnp.bfloat16)


def planned(
    queries,
    latents,
    rope_key,
    w_key,
    w_value,
    w_out,
    resid,
    gain_mix,
    w_gate,
    w_up,
    w_down,
    gain_out,
):
    z, x, y, c = coordinates()
    local_rows = queries.shape[0]
    head_count = w_key.shape[1] // NOPE
    positions = lax.axis_index("sp") * local_rows + jnp.arange(local_rows, dtype=jnp.int32)
    cosine, sine = rotary_tables(positions, ROPE, GRID_W)
    key_rot = rotate(rope_key, cosine, sine)

    half = local_rows // PAIR
    wide = jnp.concatenate(
        [latents, key_rot, jnp.zeros((local_rows, LANES - ROPE), jnp.bfloat16)], axis=1
    )
    piece = lax.dynamic_slice_in_dim(wide, c * half, half, 0)
    pair = jnp.concatenate([piece, flip(piece, dx=1)], axis=0)

    depth = w_gate.shape[0]
    cuts = w_down.shape[0] // depth
    packed = jnp.concatenate(
        [w_gate, w_up]
        + [jnp.concatenate([w_down[j * depth : (j + 1) * depth] for j in range(cuts)], axis=1)],
        axis=0,
    )
    weights = exchange_halves(packed)

    near = flip(pair, dz=1)
    far = flip(pair, dz=3)
    across_low = flip(far[:half], dz=1)
    across_high = flip(near[half:], dz=3)
    mine = [pair, near, far, across_low, across_high]
    blocks = mine + [partner(block) for block in mine]

    shaped = queries.reshape(local_rows, head_count, NOPE + ROPE)
    q_nope = shaped[:, :, :NOPE]
    q_rot = rotate(shaped[:, :, NOPE:], cosine[:, None, :], sine[:, None, :])
    heads_per_tile = LANES // NOPE
    q_list = []
    for head in range(head_count):
        part = head % heads_per_tile
        q_list.append(
            jnp.concatenate(
                [
                    jnp.pad(
                        q_nope[:, head], ((0, 0), (part * NOPE, LANES - (part + 1) * NOPE))
                    ),
                    jnp.pad(q_rot[:, head], ((0, 0), (0, LANES - ROPE))),
                ],
                axis=1,
            )
        )
    heads_own = attend(jnp.stack(q_list), blocks, w_key, w_value)

    gains = jnp.pad(three_terms(gain_mix), ((0, 13), (0, 0)))
    resid_own = jnp.concatenate([resid, gains], axis=0)
    resid_pieces = [spread(resid_own, dy, k) for dy, k in ROUNDS]
    out_other = flip(w_out, dy=1)
    w_pieces = [w_out, partner(w_out), out_other, partner(out_other)]
    heads = [spread(heads_own, dy, k) for dy, k in ROUNDS]
    hidden_in, own, theirs = mix(heads, w_pieces, resid_pieces)
    got = partner(theirs)

    cut = weights.shape[0] // 2
    w_near = flip(weights, dz=1)
    w_far = flip(weights, dz=3)
    w_low = flip(w_far[:cut], dz=1)
    w_high = flip(w_near[cut:], dz=3)
    w_mine = [weights, w_near, w_far, w_low, w_high]
    w_all = w_mine + [partner(block) for block in w_mine]
    terms = feed(hidden_in, w_all, depth)
    parts = [collect(term, dy, k) for term, (dy, k) in zip(terms, ROUNDS)]
    pre, stats = add_up(parts, own, got)
    all_stats = [stats, partner(stats), flip(stats, dy=1), flip(stats, dy=1, dc=1)]
    return finish(pre, all_stats, gain_out)


def solution(mesh):
    placed = (
        P("sp", "tp"),
        P("sp", None),
        P("sp", None),
        P(None, "tp"),
        P(None, "tp"),
        P("tp", None),
        P("sp", "tp"),
        P("tp"),
        P("sp", "tp"),
        P("sp", "tp"),
        P("tp", "sp"),
        P("tp"),
    )
    body = planned if fits_plan(mesh) else local
    return jax.shard_map(
        body, mesh=mesh, in_specs=placed, out_specs=P("sp", "tp"), check_vma=False
    )
```

```python
import functools

import jax
import jax.numpy as jnp
from jax import lax
from jax.experimental import pallas as pl
from jax.experimental.pallas import tpu as pltpu

from jax.sharding import PartitionSpec as P

NOPE = 64
ROPE = 32
VDIM = 64
GRID_W = 64


ROTARY_BASE = 10000.0
NORM_EPSILON = 1e-06
DEEP_ALPHA = 8.0**0.25
HALF_STEP = 0.5


def rotary_tables(positions, rotary_width, grid_width):
    grid_rows = (positions // grid_width).astype(jnp.float32)
    grid_cols = (positions % grid_width).astype(jnp.float32)
    freq_count = rotary_width // 4
    inverse = ROTARY_BASE ** (-jnp.arange(freq_count, dtype=jnp.float32) / freq_count)
    angle_table = jnp.concatenate(
        [grid_rows[:, None] * inverse, grid_cols[:, None] * inverse], axis=-1
    )
    return (jnp.cos(angle_table), jnp.sin(angle_table))


def rotate(vectors, cosine, sine):
    half_width = vectors.shape[-1] // 2
    leading = vectors[..., :half_width].astype(jnp.float32)
    trailing = vectors[..., half_width:].astype(jnp.float32)
    return jnp.concatenate(
        [leading * cosine - trailing * sine, leading * sine + trailing * cosine], axis=-1
    ).astype(jnp.bfloat16)


def attend_block(state, key_block, query_pair):
    maxima, totals, running = state
    key_nope, value_rows, key_rope = key_block
    q_nope, q_rope = query_pair
    head_count = q_nope.shape[1]
    rows_here = key_nope.shape[0]
    key_nope = key_nope.reshape(rows_here, head_count, -1)
    value_rows = value_rows.reshape(rows_here, head_count, -1)
    score_scale = (q_nope.shape[2] + q_rope.shape[2]) ** (-0.5)
    scores = jnp.einsum("qhd,khd->hqk", q_nope, key_nope, preferred_element_type=jnp.float32)
    scores = (
        scores + jnp.einsum("qhd,kd->hqk", q_rope, key_rope, preferred_element_type=jnp.float32)
    ) * score_scale
    new_max = jnp.maximum(maxima, jnp.max(scores, axis=-1))
    weights = jnp.exp(scores - new_max[:, :, None])
    factor = jnp.exp(maxima - new_max)
    totals = totals * factor + jnp.sum(weights, axis=-1)
    update = jnp.einsum(
        "hqk,khd->qhd", weights.astype(jnp.bfloat16), value_rows, preferred_element_type=jnp.float32
    )
    running = running * jnp.transpose(factor)[:, :, None] + update
    return (new_max, totals, running)


def block_length(length):
    block_rows = length
    while block_rows > 2048 and block_rows % 2 == 0:
        block_rows = block_rows // 2
    return block_rows


def fold_keys(state, pieces, query_pair):
    length = pieces[0].shape[0]
    block_rows = block_length(length)
    if block_rows == length:
        return attend_block(state, pieces, query_pair)
    stacked = tuple(
        (member.reshape(length // block_rows, block_rows, member.shape[1]) for member in pieces)
    )

    def one_block(partial_value, key_block):
        return (attend_block(partial_value, key_block, query_pair), None)

    state, _ = lax.scan(one_block, state, stacked)
    return state


def split_norm(rows_in, gain_row):
    width_total = rows_in.shape[1] * lax.axis_size("tp")
    row_sums, squares = lax.psum(
        (jnp.sum(rows_in, axis=1), jnp.sum(rows_in * rows_in, axis=1)), "tp"
    )
    row_mean = row_sums / width_total
    variance = squares / width_total - row_mean * row_mean
    return (
        (rows_in - row_mean[:, None]) * lax.rsqrt(variance + NORM_EPSILON)[:, None] * gain_row
    ).astype(jnp.bfloat16)


def local(
    queries,
    latents,
    rope_key,
    w_key,
    w_value,
    w_out,
    resid,
    gain_mix,
    w_gate,
    w_up,
    w_down,
    gain_out,
):
    local_rows = queries.shape[0]
    head_count = w_key.shape[1] // NOPE
    offset = lax.axis_index("sp") * local_rows
    positions = offset + jnp.arange(local_rows, dtype=jnp.int32)
    cosine, sine = rotary_tables(positions, ROPE, GRID_W)
    key_rot = rotate(rope_key, cosine, sine)
    shaped = queries.reshape(local_rows, head_count, NOPE + ROPE)
    q_nope = shaped[:, :, :NOPE]
    q_rot = rotate(shaped[:, :, NOPE:], cosine[:, None, :], sine[:, None, :])
    query_pair = (q_nope, q_rot)
    start_state = (
        jnp.full((head_count, local_rows), -jnp.inf, jnp.float32),
        jnp.zeros((head_count, local_rows), jnp.float32),
        jnp.zeros((local_rows, head_count, VDIM), jnp.float32),
    )
    quarter = local_rows // lax.axis_size("tp")
    first_row = lax.axis_index("tp") * quarter
    latent_part = lax.dynamic_slice_in_dim(latents, first_row, quarter, 0)
    rotary_part = lax.dynamic_slice_in_dim(key_rot, first_row, quarter, 0)
    latent_all, rotary_all = (
        lax.all_gather(latent_part, "sp", axis=0, tiled=True),
        lax.all_gather(rotary_part, "sp", axis=0, tiled=True),
    )
    pieces = (
        lax.all_gather(latent_all, "tp", axis=0, tiled=True),
        lax.all_gather(rotary_all, "tp", axis=0, tiled=True),
    )
    key_nope = jnp.dot(pieces[0], w_key, preferred_element_type=jnp.float32).astype(jnp.bfloat16)
    value_rows = jnp.dot(pieces[0], w_value, preferred_element_type=jnp.float32).astype(
        jnp.bfloat16
    )
    state = fold_keys(start_state, (key_nope, value_rows, pieces[1]), query_pair)
    _, totals, running = state
    heads_out = (
        (running / jnp.transpose(totals)[:, :, None])
        .reshape(local_rows, head_count * VDIM)
        .astype(jnp.bfloat16)
    )
    projected = jnp.dot(heads_out, w_out, preferred_element_type=jnp.float32)
    attn_cols = lax.psum_scatter(
        projected.astype(jnp.bfloat16), "tp", scatter_dimension=1, tiled=True
    ).astype(jnp.float32)
    hidden_in = split_norm(DEEP_ALPHA * resid.astype(jnp.float32) + attn_cols, gain_mix)
    whole_rows = lax.all_gather(hidden_in, "tp", axis=1, tiled=True)
    pieces = (
        lax.all_gather(w_gate, "sp", axis=0, tiled=True),
        lax.all_gather(w_up, "sp", axis=0, tiled=True),
    )
    gate_sum = jnp.dot(whole_rows, pieces[0], preferred_element_type=jnp.float32)
    up_sum = jnp.dot(whole_rows, pieces[1], preferred_element_type=jnp.float32)
    hidden = (jax.nn.silu(gate_sum) * up_sum).astype(jnp.bfloat16)
    down_terms = jnp.dot(
        hidden, lax.all_gather(w_down, "sp", axis=1, tiled=True), preferred_element_type=jnp.float32
    )
    mixer_cols = lax.psum_scatter(
        down_terms.astype(jnp.bfloat16), "tp", scatter_dimension=1, tiled=True
    ).astype(jnp.float32)
    return split_norm(DEEP_ALPHA * hidden_in.astype(jnp.float32) + HALF_STEP * mixer_cols, gain_out)


RING = 4
PAIR = 2
LANES = 128
BOTH = ("sp", "tp")
VMEM = pl.BlockSpec(memory_space=pltpu.VMEM)
HBM = pl.BlockSpec(memory_space=pl.ANY)
PARAMS = pltpu.CompilerParams(vmem_limit_bytes=20 * 1024 * 1024)


def fits_plan(mesh):
    return mesh.shape["sp"] == RING * PAIR and mesh.shape["tp"] == PAIR * PAIR


def sp_index(r, p):
    return (r // PAIR) * PAIR * PAIR + p * PAIR + r % PAIR


def move(array, where):
    pairs = []
    for r in range(RING):
        for p in range(PAIR):
            for y in range(PAIR):
                for c in range(PAIR):
                    target = where(r, p, y, c)
                    if target is None:
                        continue
                    to_r, to_p, to_y, to_c = target
                    here = sp_index(r, p) * PAIR * PAIR + y * PAIR + c
                    there = sp_index(to_r, to_p) * PAIR * PAIR + to_y * PAIR + to_c
                    pairs.append((here, there))
    return lax.ppermute(array, BOTH, pairs)


def flip(array, dr=0, dp=0, dy=0, dc=0):
    return move(array, lambda r, p, y, c: (r ^ dr, p ^ dp, y ^ dy, c ^ dc))


def partner(array):
    return flip(array, dc=1)


def exchange_halves(array):
    return move(array, lambda r, p, y, c: (r, c, y, p) if c != p else None)


ROUNDS = ((0, 0), (0, 1), (1, 0), (1, 1))


def spread(array, dy, k):
    return move(array, lambda r, p, y, c: (r, c ^ k, y ^ dy, p))


def coordinates():
    sp = lax.axis_index("sp")
    tp = lax.axis_index("tp")
    ring = (sp // (PAIR * PAIR)) * PAIR + sp % PAIR
    return (ring, (sp // PAIR) % PAIR, tp // PAIR, tp % PAIR)


def other(bit):
    return 1 - bit


def round_block(dy, k, p, y):
    row = other(y) if dy else y
    column = other(p) if k else p
    return row * PAIR + column


def query_tiles(queries, cosine, sine):
    rows = queries.shape[0]
    half = ROPE // 2
    heads_per_tile = LANES // NOPE
    tiles = []
    for head in range(queries.shape[1] // (NOPE + ROPE)):
        start = head * (NOPE + ROPE)
        plain = queries[:, start : start + NOPE]
        leading = queries[:, start + NOPE : start + NOPE + half]
        trailing = queries[:, start + NOPE + half : start + NOPE + ROPE]
        part = head % heads_per_tile
        pieces = [plain]
        if part:
            pieces.insert(0, jnp.zeros((rows, part * NOPE), jnp.float32))
        if part < heads_per_tile - 1:
            pieces.append(jnp.zeros((rows, LANES - (part + 1) * NOPE), jnp.float32))
        pieces.append(leading * cosine - trailing * sine)
        pieces.append(leading * sine + trailing * cosine)
        pieces.append(jnp.zeros((rows, LANES - ROPE), jnp.float32))
        tiles.append(jnp.concatenate(pieces, axis=1).astype(jnp.bfloat16))
    return tiles


def attention_kernel(scale, n_blocks, *refs):
    first = refs[:3]
    blocks = refs[3 : 3 + n_blocks]
    weights = refs[3 + n_blocks : 5 + n_blocks]
    out_hbm, k_scr, v_scr, x_scr, q_ref, cos_ref, sin_ref, wk_ref, wv_ref, out_ref, sems = refs[
        5 + n_blocks :
    ]
    rank = wk_ref.shape[0]
    tiles = wk_ref.shape[1] // LANES
    copies = []
    early = []
    for at, (ref, scr) in enumerate(zip(first, (q_ref, cos_ref, sin_ref))):
        early.append(pltpu.make_async_copy(ref, scr, sems.at[n_blocks + at]))
    for at, (ref, scr) in enumerate(zip(weights, (wk_ref, wv_ref))):
        copies.append(pltpu.make_async_copy(ref, scr, sems.at[n_blocks + 3 + at]))
    for copy in early + copies:
        copy.start()
    offset = 0
    for at, ref in enumerate(blocks):
        rows = ref.shape[0]
        copy = pltpu.make_async_copy(ref, x_scr.at[pl.ds(offset, rows)], sems.at[at])
        copy.start()
        copies.append(copy)
        offset += rows
    for copy in early:
        copy.wait()
    q_tiles = query_tiles(q_ref[...].astype(jnp.float32), cos_ref[...], sin_ref[...])
    for copy in copies:
        copy.wait()
    lat = x_scr[:, :rank]
    keys = jnp.dot(lat, wk_ref[...], preferred_element_type=jnp.float32).astype(jnp.bfloat16)
    for tile in range(tiles):
        k_scr[tile, :, :LANES] = keys[:, tile * LANES : (tile + 1) * LANES]
        k_scr[tile, :, LANES:] = x_scr[:, rank:]
    v_scr[...] = jnp.dot(lat, wv_ref[...], preferred_element_type=jnp.float32).astype(jnp.bfloat16)
    heads_per_tile = LANES // NOPE
    for tile in range(tiles):
        merged = None
        for part in range(heads_per_tile):
            scores = lax.dot_general(
                q_tiles[tile * heads_per_tile + part],
                k_scr[tile],
                (((1,), (1,)), ((), ())),
                preferred_element_type=jnp.float32,
            )
            top = jnp.max(scores, axis=-1, keepdims=True)
            weights = jnp.exp((scores - top) * scale)
            total = jnp.sum(weights, axis=-1, keepdims=True)
            update = jnp.dot(
                weights.astype(jnp.bfloat16),
                v_scr[:, tile * LANES : (tile + 1) * LANES],
                preferred_element_type=jnp.float32,
            )
            update = update / total
            lane = lax.broadcasted_iota(jnp.int32, update.shape, 1)
            mine = (lane >= part * NOPE) & (lane < (part + 1) * NOPE)
            merged = update if merged is None else jnp.where(mine, update, merged)
        out_ref[:, tile * LANES : (tile + 1) * LANES] = merged.astype(jnp.bfloat16)
    done = pltpu.make_async_copy(out_ref, out_hbm, sems.at[0])
    done.start()
    done.wait()


def attend(queries, cosine, sine, blocks, w_key, w_value):
    keys = sum(block.shape[0] for block in blocks)
    tiles = w_key.shape[1] // LANES
    rows = queries.shape[0]
    return pl.pallas_call(
        functools.partial(attention_kernel, (NOPE + ROPE) ** (-0.5), len(blocks)),
        out_shape=jax.ShapeDtypeStruct((rows, w_value.shape[1]), jnp.bfloat16),
        in_specs=[HBM] * (len(blocks) + 5),
        out_specs=HBM,
        scratch_shapes=[
            pltpu.VMEM((tiles, keys, 2 * LANES), jnp.bfloat16),
            pltpu.VMEM((keys, w_value.shape[1]), jnp.bfloat16),
            pltpu.VMEM((keys, blocks[0].shape[1]), jnp.bfloat16),
            pltpu.VMEM(queries.shape, queries.dtype),
            pltpu.VMEM(cosine.shape, cosine.dtype),
            pltpu.VMEM(sine.shape, sine.dtype),
            pltpu.VMEM(w_key.shape, w_key.dtype),
            pltpu.VMEM(w_value.shape, w_value.dtype),
            pltpu.VMEM((rows, w_value.shape[1]), jnp.bfloat16),
            pltpu.SemaphoreType.DMA((len(blocks) + 5,)),
        ],
        compiler_params=PARAMS,
        name="attend",
    )(queries, cosine, sine, *blocks, w_key, w_value)


def mix_kernel(*refs):
    heads = refs[0:4]
    w_refs = refs[4:8]
    resid_refs = refs[8:12]
    out_hbm, hid_ref, h_scr, w_scr, in_scr, res_scr, gain_scr, sems = refs[12:]
    _, p, y, c = coordinates()
    turned = (p + c) % PAIR
    small = []
    large = []
    for j in range(4):
        slot = j + turned * (1 - 2 * (j % PAIR))
        small.append(pltpu.make_async_copy(resid_refs[j], in_scr.at[j], sems.at[0, j]))
        large.append(pltpu.make_async_copy(heads[j], h_scr.at[j], sems.at[1, j]))
        large.append(pltpu.make_async_copy(w_refs[j], w_scr.at[slot], sems.at[2, j]))
    for copy in small + large:
        copy.start()
    for copy in small:
        copy.wait()
    rows = hid_ref.shape[0]
    width = resid_refs[0].shape[1]
    for j, (dy, k) in enumerate(ROUNDS):
        columns = pl.ds(pl.multiple_of(round_block(dy, k, p, y) * width, width), width)
        res_scr[:, columns] = DEEP_ALPHA * in_scr[j, :rows, :].astype(jnp.float32)
        gains = in_scr[j, rows:, :].astype(jnp.float32)
        gain_scr[:, columns] = gains[0:1] + gains[1:2] + gains[2:3]
    for copy in large:
        copy.wait()
    chunk = rows // 4
    outs = []
    for start in range(0, rows, chunk):
        span = slice(start, start + chunk)
        mixed = res_scr[span, :]
        for j in range(4):
            mixed = mixed + jnp.dot(h_scr[j, span, :], w_scr[j], preferred_element_type=jnp.float32)
        mean = jnp.mean(mixed, axis=1, keepdims=True)
        variance = jnp.mean(mixed * mixed, axis=1, keepdims=True) - mean * mean
        hid_ref[span, :] = (
            (mixed - mean) * lax.rsqrt(variance + NORM_EPSILON) * gain_scr[...]
        ).astype(jnp.bfloat16)
        part = pl.ds(start, chunk)
        copy = pltpu.make_async_copy(hid_ref.at[part], out_hbm.at[part], sems.at[3, len(outs)])
        copy.start()
        outs.append(copy)
    for copy in outs:
        copy.wait()


def mix(heads, w_pieces, resid_pieces):
    rows, share = heads[0].shape
    depth, width_total = w_pieces[0].shape
    return pl.pallas_call(
        mix_kernel,
        out_shape=jax.ShapeDtypeStruct((rows, width_total), jnp.bfloat16),
        in_specs=[HBM] * 12,
        out_specs=HBM,
        scratch_shapes=[
            pltpu.VMEM((rows, width_total), jnp.bfloat16),
            pltpu.VMEM((4, rows, share), jnp.bfloat16),
            pltpu.VMEM((4, depth, width_total), jnp.bfloat16),
            pltpu.VMEM((4,) + resid_pieces[0].shape, jnp.bfloat16),
            pltpu.VMEM((rows, width_total), jnp.float32),
            pltpu.VMEM((1, width_total), jnp.float32),
            pltpu.SemaphoreType.DMA((4, 4)),
        ],
        compiler_params=PARAMS,
        name="mix",
    )(*heads, *w_pieces, *resid_pieces)


def homes(r):
    high = r // PAIR
    low = r % PAIR
    return ((high, low), (high, other(low)), (other(high), low), (other(high), other(low)))


def up_kernel(own_ref, got_ref, *refs):
    gates = refs[:4]
    ups = refs[4:8]
    out_hbm, out_ref, h_scr, g_scr, u_scr, sems = refs[8:]
    r, _, _, c = coordinates()
    depth, units = gates[0].shape
    rows = own_ref.shape[0]
    copies = []
    for at in range(4):
        span = pl.ds(at * depth, depth)
        copies.append(pltpu.make_async_copy(gates[at], g_scr.at[span], sems.at[0, at]))
    for at in range(4):
        span = pl.ds(at * depth, depth)
        copies.append(pltpu.make_async_copy(ups[at], u_scr.at[span], sems.at[1, at]))
    for at, (row, column) in enumerate(homes(r)):
        block = row * PAIR * PAIR + c * PAIR + column
        columns = pl.ds(pl.multiple_of(block * depth, depth), depth)
        span = pl.ds(at * depth, depth)
        for side, ref in enumerate((own_ref, got_ref)):
            copies.append(
                pltpu.make_async_copy(
                    ref.at[:, columns],
                    h_scr.at[pl.ds(side * rows, rows), span],
                    sems.at[2 + side, at],
                )
            )
    for copy in copies:
        copy.start()
    for copy in copies[:4] + copies[8:]:
        copy.wait()
    hid = h_scr[...]
    out_ref[:, :units] = jnp.dot(hid, g_scr[...], preferred_element_type=jnp.float32).astype(
        jnp.bfloat16
    )
    outs = []
    for side in range(2):
        columns = pl.ds(side * units, units)
        outs.append(
            pltpu.make_async_copy(
                out_ref.at[:, columns], out_hbm.at[:, columns], sems.at[4, side]
            )
        )
    outs[0].start()
    for copy in copies[4:8]:
        copy.wait()
    out_ref[:, units:] = jnp.dot(hid, u_scr[...], preferred_element_type=jnp.float32).astype(
        jnp.bfloat16
    )
    outs[1].start()
    for copy in outs:
        copy.wait()


def feed_up(own, got, gates, ups):
    rows = own.shape[0]
    depth, units = gates[0].shape
    return pl.pallas_call(
        up_kernel,
        out_shape=jax.ShapeDtypeStruct((PAIR * rows, 2 * units), jnp.bfloat16),
        in_specs=[HBM] * 10,
        out_specs=HBM,
        scratch_shapes=[
            pltpu.VMEM((PAIR * rows, 2 * units), jnp.bfloat16),
            pltpu.VMEM((PAIR * rows, 4 * depth), jnp.bfloat16),
            pltpu.VMEM((4 * depth, units), jnp.bfloat16),
            pltpu.VMEM((4 * depth, units), jnp.bfloat16),
            pltpu.SemaphoreType.DMA((5, 4)),
        ],
        compiler_params=PARAMS,
        name="feed_up",
    )(own, got, *gates, *ups)


def down_kernel(own_ref, got_ref, *refs):
    downs = refs[:4]
    outs = refs[4:8]
    o_scr, a_scr, d_scr, own_scr, got_scr, sems = refs[8:]
    r, p, y, c = coordinates()
    depth = downs[0].shape[1]
    rows, units = a_scr.shape[1:]
    copies = []
    for at, (row, column) in enumerate(homes(r)):
        columns = pl.ds(pl.multiple_of(column * depth, depth), depth)
        copies.append(
            pltpu.make_async_copy(downs[at], d_scr.at[row, :, columns], sems.at[at])
        )
    inputs = [
        pltpu.make_async_copy(own_ref, own_scr, sems.at[4]),
        pltpu.make_async_copy(got_ref, got_scr, sems.at[5]),
    ]
    for copy in inputs + copies:
        copy.start()
    for copy in inputs:
        copy.wait()
    for side in range(2):
        mine = pl.ds(side * rows, rows)
        theirs = pl.ds((1 - side) * rows, rows)
        gate = own_scr[mine, :units].astype(jnp.float32) + got_scr[theirs, :units].astype(
            jnp.float32
        )
        up = own_scr[mine, units:].astype(jnp.float32) + got_scr[theirs, units:].astype(
            jnp.float32
        )
        group = c if side == 0 else other(c)
        a_scr[group] = (gate / (1.0 + jnp.exp(-gate)) * up).astype(jnp.bfloat16)
    for copy in copies:
        copy.wait()
    stores = []
    for j, (dy, dp) in enumerate(ROUNDS):
        group = other(p) if dp else p
        row = other(y) if dy else y
        o_scr[j] = jnp.dot(a_scr[group], d_scr[row], preferred_element_type=jnp.float32).astype(
            jnp.bfloat16
        )
        copy = pltpu.make_async_copy(o_scr.at[j], outs[j], sems.at[6 + j])
        copy.start()
        stores.append(copy)
    for copy in stores:
        copy.wait()


def feed_down(own, got, downs):
    rows = own.shape[0] // PAIR
    units, depth = downs[0].shape
    block = jax.ShapeDtypeStruct((rows, PAIR * depth), jnp.bfloat16)
    return pl.pallas_call(
        down_kernel,
        out_shape=(block,) * 4,
        in_specs=[HBM] * 6,
        out_specs=(HBM,) * 4,
        scratch_shapes=[
            pltpu.VMEM((4, rows, PAIR * depth), jnp.bfloat16),
            pltpu.VMEM((PAIR, rows, units), jnp.bfloat16),
            pltpu.VMEM((PAIR, units, PAIR * depth), jnp.bfloat16),
            pltpu.VMEM(own.shape, jnp.bfloat16),
            pltpu.VMEM(own.shape, jnp.bfloat16),
            pltpu.SemaphoreType.DMA((10,)),
        ],
        compiler_params=PARAMS,
        name="feed_down",
    )(own, got, *downs)


def sum_kernel(own_ref, got_ref, *refs):
    terms = refs[:4]
    pre_ref, stat_ref, t_scr, h_scr, sems = refs[4:]
    _, p, y, c = coordinates()
    rows, width = pre_ref.shape
    copies = []
    for j in range(4):
        copy = pltpu.make_async_copy(terms[j], t_scr.at[j], sems.at[j])
        copy.start()
        copies.append(copy)
    columns = pl.ds(pl.multiple_of((y * PAIR + c) * width, width), width)
    for side, ref in enumerate((own_ref, got_ref)):
        copy = pltpu.make_async_copy(ref.at[:, columns], h_scr.at[side], sems.at[4 + side])
        copy.start()
        copies.append(copy)
    for copy in copies:
        copy.wait()
    total = jnp.zeros((rows, width), jnp.float32)
    for j in range(4):
        total = total + t_scr[j].astype(jnp.float32)
    skip = h_scr[(p + c) % PAIR].astype(jnp.float32)
    pre = DEEP_ALPHA * skip + HALF_STEP * total
    pre_ref[...] = pre
    lane = lax.broadcasted_iota(jnp.int32, (rows, LANES), 1)
    sums = jnp.sum(pre, axis=1, keepdims=True)
    squares = jnp.sum(pre * pre, axis=1, keepdims=True)
    table = jnp.where(lane == 0, sums, jnp.where(lane == 1, squares, 0.0))
    stat_ref[...] = jnp.transpose(table)[: stat_ref.shape[0], :]


def add_up(own, got, terms):
    rows, width = terms[0].shape
    return pl.pallas_call(
        sum_kernel,
        out_shape=(
            jax.ShapeDtypeStruct((rows, width), jnp.float32),
            jax.ShapeDtypeStruct((8, rows), jnp.float32),
        ),
        in_specs=[HBM] * 6,
        out_specs=(VMEM,) * 2,
        scratch_shapes=[
            pltpu.VMEM((4, rows, width), jnp.bfloat16),
            pltpu.VMEM((2, rows, width), jnp.bfloat16),
            pltpu.SemaphoreType.DMA((6,)),
        ],
        compiler_params=PARAMS,
        name="add_up",
    )(own, got, *terms)


def norm_kernel(width_total, pre_ref, a_ref, b_ref, c_ref, d_ref, gain_ref, out_ref):
    stats = a_ref[...] + b_ref[...] + c_ref[...] + d_ref[...]
    tall = jnp.concatenate(
        [stats, jnp.zeros((LANES - stats.shape[0], stats.shape[1]), jnp.float32)], axis=0
    )
    table = jnp.transpose(tall)
    mean = table[:, 0:1] / width_total
    variance = table[:, 1:2] / width_total - mean * mean
    out_ref[...] = (
        (pre_ref[...] - mean) * lax.rsqrt(variance + NORM_EPSILON) * gain_ref[...]
    ).astype(jnp.bfloat16)


def finish(pre, stats, gain):
    return pl.pallas_call(
        functools.partial(norm_kernel, pre.shape[1] * PAIR * PAIR),
        out_shape=jax.ShapeDtypeStruct(pre.shape, jnp.bfloat16),
        in_specs=[VMEM] * 6,
        out_specs=VMEM,
        compiler_params=PARAMS,
        name="finish",
    )(pre, *stats, gain.reshape(1, -1))


def three_terms(gain):
    first = lax.reduce_precision(gain, 8, 7)
    left = gain - first
    second = lax.reduce_precision(left, 8, 7)
    third = left - second
    return jnp.stack([first, second, third]).astype(jnp.bfloat16)


def planned(*arrays):
    return planned_steps(*arrays)


def planned_steps(
    queries,
    latents,
    rope_key,
    w_key,
    w_value,
    w_out,
    resid,
    gain_mix,
    w_gate,
    w_up,
    w_down,
    gain_out,
):
    _, p, _, c = coordinates()
    local_rows = queries.shape[0]
    positions = lax.axis_index("sp") * local_rows + jnp.arange(local_rows, dtype=jnp.int32)
    cosine, sine = rotary_tables(positions, ROPE, GRID_W)
    key_rot = rotate(rope_key, cosine, sine)

    half = local_rows // PAIR
    wide = jnp.concatenate(
        [latents, key_rot, jnp.zeros((local_rows, LANES - ROPE), jnp.bfloat16)], axis=1
    )
    piece = lax.dynamic_slice_in_dim(wide, c * half, half, 0)
    near = flip(piece, dp=1)
    far = flip(piece, dr=2, dp=1)
    cut = half // 2
    across_low = flip(far[:cut], dp=1)
    across_high = flip(near[cut:], dr=2, dp=1)
    crossed = flip(piece, dr=1)
    first = jnp.concatenate([near, far], axis=0)
    first = [piece, first, crossed, flip(first, dr=1)]
    last = jnp.concatenate([across_low, across_high], axis=0)
    last = [last, flip(last, dr=1)]
    first = jnp.concatenate(first, axis=0)
    first = [first, partner(first)]
    last = jnp.concatenate(last, axis=0)
    last = [last, partner(last)]
    blocks = first + last

    shards = {"g": w_gate, "u": w_up, "d": w_down}
    swapped = {}
    for name, shard in shards.items():
        swapped[name] = exchange_halves(shard)

    heads_own = attend(queries, cosine, sine, blocks, w_key, w_value)
    swapped["d"], heads_own = lax.optimization_barrier((swapped["d"], heads_own))
    gathered = []
    for name, shard in shards.items():
        shard = jnp.where(p == c, shard, swapped[name])
        w_near = flip(shard, dr=1)
        w_far = flip(shard, dr=2)
        w_across = flip(w_far, dr=1)
        gathered.append([shard, w_near, w_far, w_across])


    gains = jnp.pad(three_terms(gain_mix), ((0, 13), (0, 0)))
    resid_own = jnp.concatenate([resid, gains], axis=0)
    resid_pieces = []
    for dy, k in ROUNDS:
        resid_pieces.append(spread(resid_own, dy, k))
    out_other = flip(w_out, dy=1)
    w_partner = partner(w_out)
    out_last = partner(out_other)
    w_pieces = [w_out, w_partner, out_other, out_last]
    heads = []
    for dy, k in ROUNDS:
        heads.append(spread(heads_own, dy, k))
    hidden = mix(heads, w_pieces, resid_pieces)
    got = partner(hidden)
    sums = feed_up(hidden, got, gathered[0], gathered[1])
    sums_got = partner(sums)
    terms = list(feed_down(sums, sums_got, gathered[2]))
    for at, (dy, dp) in enumerate(ROUNDS):
        if dy or dp:
            terms[at] = flip(terms[at], dp=dp, dy=dy)
    pre, stats = add_up(hidden, got, terms)
    stat_y = flip(stats, dy=1)
    stat_yc = flip(stats, dy=1, dc=1)
    stat_c = partner(stats)
    return finish(pre, [stats, stat_c, stat_y, stat_yc], gain_out)


def solution(mesh):
    placed = (
        P("sp", "tp"),
        P("sp", None),
        P("sp", None),
        P(None, "tp"),
        P(None, "tp"),
        P("tp", None),
        P("sp", "tp"),
        P("tp"),
        P("sp", "tp"),
        P("sp", "tp"),
        P("tp", "sp"),
        P("tp"),
    )
    body = planned if fits_plan(mesh) else local
    return jax.shard_map(
        body, mesh=mesh, in_specs=placed, out_specs=P("sp", "tp"), check_vma=False
    )
```

```python
import functools

import jax
import jax.numpy as jnp
from jax import lax
from jax.experimental import pallas as pl
from jax.experimental.pallas import tpu as pltpu

from jax.sharding import PartitionSpec as P

NOPE = 64
ROPE = 32
VDIM = 64
GRID_W = 64


ROTARY_BASE = 10000.0
NORM_EPSILON = 1e-06
DEEP_ALPHA = 8.0**0.25
HALF_STEP = 0.5


def rotary_tables(positions, rotary_width, grid_width):
    grid_rows = (positions // grid_width).astype(jnp.float32)
    grid_cols = (positions % grid_width).astype(jnp.float32)
    freq_count = rotary_width // 4
    inverse = ROTARY_BASE ** (-jnp.arange(freq_count, dtype=jnp.float32) / freq_count)
    angle_table = jnp.concatenate(
        [grid_rows[:, None] * inverse, grid_cols[:, None] * inverse], axis=-1
    )
    return (jnp.cos(angle_table), jnp.sin(angle_table))


def rotate(vectors, cosine, sine):
    half_width = vectors.shape[-1] // 2
    leading = vectors[..., :half_width].astype(jnp.float32)
    trailing = vectors[..., half_width:].astype(jnp.float32)
    return jnp.concatenate(
        [leading * cosine - trailing * sine, leading * sine + trailing * cosine], axis=-1
    ).astype(jnp.bfloat16)


def attend_block(state, key_block, query_pair):
    maxima, totals, running = state
    key_nope, value_rows, key_rope = key_block
    q_nope, q_rope = query_pair
    head_count = q_nope.shape[1]
    rows_here = key_nope.shape[0]
    key_nope = key_nope.reshape(rows_here, head_count, -1)
    value_rows = value_rows.reshape(rows_here, head_count, -1)
    score_scale = (q_nope.shape[2] + q_rope.shape[2]) ** (-0.5)
    scores = jnp.einsum("qhd,khd->hqk", q_nope, key_nope, preferred_element_type=jnp.float32)
    scores = (
        scores + jnp.einsum("qhd,kd->hqk", q_rope, key_rope, preferred_element_type=jnp.float32)
    ) * score_scale
    new_max = jnp.maximum(maxima, jnp.max(scores, axis=-1))
    weights = jnp.exp(scores - new_max[:, :, None])
    factor = jnp.exp(maxima - new_max)
    totals = totals * factor + jnp.sum(weights, axis=-1)
    update = jnp.einsum(
        "hqk,khd->qhd", weights.astype(jnp.bfloat16), value_rows, preferred_element_type=jnp.float32
    )
    running = running * jnp.transpose(factor)[:, :, None] + update
    return (new_max, totals, running)


def block_length(length):
    block_rows = length
    while block_rows > 2048 and block_rows % 2 == 0:
        block_rows = block_rows // 2
    return block_rows


def fold_keys(state, pieces, query_pair):
    length = pieces[0].shape[0]
    block_rows = block_length(length)
    if block_rows == length:
        return attend_block(state, pieces, query_pair)
    stacked = tuple(
        (member.reshape(length // block_rows, block_rows, member.shape[1]) for member in pieces)
    )

    def one_block(partial_value, key_block):
        return (attend_block(partial_value, key_block, query_pair), None)

    state, _ = lax.scan(one_block, state, stacked)
    return state


def split_norm(rows_in, gain_row):
    width_total = rows_in.shape[1] * lax.axis_size("tp")
    row_sums, squares = lax.psum(
        (jnp.sum(rows_in, axis=1), jnp.sum(rows_in * rows_in, axis=1)), "tp"
    )
    row_mean = row_sums / width_total
    variance = squares / width_total - row_mean * row_mean
    return (
        (rows_in - row_mean[:, None]) * lax.rsqrt(variance + NORM_EPSILON)[:, None] * gain_row
    ).astype(jnp.bfloat16)


def local(
    queries,
    latents,
    rope_key,
    w_key,
    w_value,
    w_out,
    resid,
    gain_mix,
    w_gate,
    w_up,
    w_down,
    gain_out,
):
    local_rows = queries.shape[0]
    head_count = w_key.shape[1] // NOPE
    offset = lax.axis_index("sp") * local_rows
    positions = offset + jnp.arange(local_rows, dtype=jnp.int32)
    cosine, sine = rotary_tables(positions, ROPE, GRID_W)
    key_rot = rotate(rope_key, cosine, sine)
    shaped = queries.reshape(local_rows, head_count, NOPE + ROPE)
    q_nope = shaped[:, :, :NOPE]
    q_rot = rotate(shaped[:, :, NOPE:], cosine[:, None, :], sine[:, None, :])
    query_pair = (q_nope, q_rot)
    start_state = (
        jnp.full((head_count, local_rows), -jnp.inf, jnp.float32),
        jnp.zeros((head_count, local_rows), jnp.float32),
        jnp.zeros((local_rows, head_count, VDIM), jnp.float32),
    )
    quarter = local_rows // lax.axis_size("tp")
    first_row = lax.axis_index("tp") * quarter
    latent_part = lax.dynamic_slice_in_dim(latents, first_row, quarter, 0)
    rotary_part = lax.dynamic_slice_in_dim(key_rot, first_row, quarter, 0)
    latent_all, rotary_all = (
        lax.all_gather(latent_part, "sp", axis=0, tiled=True),
        lax.all_gather(rotary_part, "sp", axis=0, tiled=True),
    )
    pieces = (
        lax.all_gather(latent_all, "tp", axis=0, tiled=True),
        lax.all_gather(rotary_all, "tp", axis=0, tiled=True),
    )
    key_nope = jnp.dot(pieces[0], w_key, preferred_element_type=jnp.float32).astype(jnp.bfloat16)
    value_rows = jnp.dot(pieces[0], w_value, preferred_element_type=jnp.float32).astype(
        jnp.bfloat16
    )
    state = fold_keys(start_state, (key_nope, value_rows, pieces[1]), query_pair)
    _, totals, running = state
    heads_out = (
        (running / jnp.transpose(totals)[:, :, None])
        .reshape(local_rows, head_count * VDIM)
        .astype(jnp.bfloat16)
    )
    projected = jnp.dot(heads_out, w_out, preferred_element_type=jnp.float32)
    attn_cols = lax.psum_scatter(
        projected.astype(jnp.bfloat16), "tp", scatter_dimension=1, tiled=True
    ).astype(jnp.float32)
    hidden_in = split_norm(DEEP_ALPHA * resid.astype(jnp.float32) + attn_cols, gain_mix)
    whole_rows = lax.all_gather(hidden_in, "tp", axis=1, tiled=True)
    pieces = (
        lax.all_gather(w_gate, "sp", axis=0, tiled=True),
        lax.all_gather(w_up, "sp", axis=0, tiled=True),
    )
    gate_sum = jnp.dot(whole_rows, pieces[0], preferred_element_type=jnp.float32)
    up_sum = jnp.dot(whole_rows, pieces[1], preferred_element_type=jnp.float32)
    hidden = (jax.nn.silu(gate_sum) * up_sum).astype(jnp.bfloat16)
    down_terms = jnp.dot(
        hidden, lax.all_gather(w_down, "sp", axis=1, tiled=True), preferred_element_type=jnp.float32
    )
    mixer_cols = lax.psum_scatter(
        down_terms.astype(jnp.bfloat16), "tp", scatter_dimension=1, tiled=True
    ).astype(jnp.float32)
    return split_norm(DEEP_ALPHA * hidden_in.astype(jnp.float32) + HALF_STEP * mixer_cols, gain_out)


RING = 4
PAIR = 2
LANES = 128
BOTH = ("sp", "tp")
VMEM = pl.BlockSpec(memory_space=pltpu.VMEM)
HBM = pl.BlockSpec(memory_space=pl.ANY)
PARAMS = pltpu.CompilerParams(vmem_limit_bytes=20 * 1024 * 1024)


def fits_plan(mesh):
    return mesh.shape["sp"] == RING * PAIR and mesh.shape["tp"] == PAIR * PAIR


def sp_index(r, p):
    return (r // PAIR) * PAIR * PAIR + p * PAIR + r % PAIR


def move(array, where):
    pairs = []
    for r in range(RING):
        for p in range(PAIR):
            for y in range(PAIR):
                for c in range(PAIR):
                    target = where(r, p, y, c)
                    if target is None:
                        continue
                    to_r, to_p, to_y, to_c = target
                    here = sp_index(r, p) * PAIR * PAIR + y * PAIR + c
                    there = sp_index(to_r, to_p) * PAIR * PAIR + to_y * PAIR + to_c
                    pairs.append((here, there))
    return lax.ppermute(array, BOTH, pairs)


def flip(array, dr=0, dp=0, dy=0, dc=0):
    return move(array, lambda r, p, y, c: (r ^ dr, p ^ dp, y ^ dy, c ^ dc))


def partner(array):
    return flip(array, dc=1)


ROUNDS = ((0, 0), (0, 1), (1, 0), (1, 1))


def spread(array, dy, k):
    return move(array, lambda r, p, y, c: (r, c ^ k, y ^ dy, p))


def coordinates():
    sp = lax.axis_index("sp")
    tp = lax.axis_index("tp")
    ring = (sp // (PAIR * PAIR)) * PAIR + sp % PAIR
    return (ring, (sp // PAIR) % PAIR, tp // PAIR, tp % PAIR)


def other(bit):
    return 1 - bit


def round_block(dy, k, p, y):
    row = other(y) if dy else y
    column = other(p) if k else p
    return row * PAIR + column


def query_tiles(queries, cosine, sine):
    rows = queries.shape[0]
    half = ROPE // 2
    heads_per_tile = LANES // NOPE
    tiles = []
    for head in range(queries.shape[1] // (NOPE + ROPE)):
        start = head * (NOPE + ROPE)
        plain = queries[:, start : start + NOPE]
        leading = queries[:, start + NOPE : start + NOPE + half]
        trailing = queries[:, start + NOPE + half : start + NOPE + ROPE]
        part = head % heads_per_tile
        pieces = [plain]
        if part:
            pieces.insert(0, jnp.zeros((rows, part * NOPE), jnp.float32))
        if part < heads_per_tile - 1:
            pieces.append(jnp.zeros((rows, LANES - (part + 1) * NOPE), jnp.float32))
        pieces.append(leading * cosine - trailing * sine)
        pieces.append(leading * sine + trailing * cosine)
        pieces.append(jnp.zeros((rows, LANES - ROPE), jnp.float32))
        tiles.append(jnp.concatenate(pieces, axis=1).astype(jnp.bfloat16))
    return tiles


def attention_kernel(scale, n_blocks, *refs):
    first = refs[:3]
    blocks = refs[3 : 3 + n_blocks]
    weights = refs[3 + n_blocks : 5 + n_blocks]
    out_hbm, k_scr, v_scr, x_scr, q_ref, cos_ref, sin_ref, wk_ref, wv_ref, out_ref, sems = refs[
        5 + n_blocks :
    ]
    rank = wk_ref.shape[0]
    tiles = wk_ref.shape[1] // LANES
    copies = []
    early = []
    for at, (ref, scr) in enumerate(zip(first, (q_ref, cos_ref, sin_ref))):
        early.append(pltpu.make_async_copy(ref, scr, sems.at[n_blocks + at]))
    for at, (ref, scr) in enumerate(zip(weights, (wk_ref, wv_ref))):
        copies.append(pltpu.make_async_copy(ref, scr, sems.at[n_blocks + 3 + at]))
    for copy in early + copies:
        copy.start()
    offset = 0
    for at, ref in enumerate(blocks):
        rows = ref.shape[0]
        copy = pltpu.make_async_copy(ref, x_scr.at[pl.ds(offset, rows)], sems.at[at])
        copy.start()
        copies.append(copy)
        offset += rows
    for copy in early:
        copy.wait()
    q_tiles = query_tiles(q_ref[...].astype(jnp.float32), cos_ref[...], sin_ref[...])
    for copy in copies:
        copy.wait()
    lat = x_scr[:, :rank]
    keys = jnp.dot(lat, wk_ref[...], preferred_element_type=jnp.float32).astype(jnp.bfloat16)
    for tile in range(tiles):
        k_scr[tile, :, :LANES] = keys[:, tile * LANES : (tile + 1) * LANES]
        k_scr[tile, :, LANES:] = x_scr[:, rank:]
    v_scr[...] = jnp.dot(lat, wv_ref[...], preferred_element_type=jnp.float32).astype(jnp.bfloat16)
    heads_per_tile = LANES // NOPE
    for tile in range(tiles):
        merged = None
        for part in range(heads_per_tile):
            scores = lax.dot_general(
                q_tiles[tile * heads_per_tile + part],
                k_scr[tile],
                (((1,), (1,)), ((), ())),
                preferred_element_type=jnp.float32,
            )
            top = jnp.max(scores, axis=-1, keepdims=True)
            weights = jnp.exp((scores - top) * scale)
            total = jnp.sum(weights, axis=-1, keepdims=True)
            update = jnp.dot(
                weights.astype(jnp.bfloat16),
                v_scr[:, tile * LANES : (tile + 1) * LANES],
                preferred_element_type=jnp.float32,
            )
            update = update / total
            lane = lax.broadcasted_iota(jnp.int32, update.shape, 1)
            mine = (lane >= part * NOPE) & (lane < (part + 1) * NOPE)
            merged = update if merged is None else jnp.where(mine, update, merged)
        out_ref[:, tile * LANES : (tile + 1) * LANES] = merged.astype(jnp.bfloat16)
    done = pltpu.make_async_copy(out_ref, out_hbm, sems.at[0])
    done.start()
    done.wait()


def attend(queries, cosine, sine, blocks, w_key, w_value):
    keys = sum(block.shape[0] for block in blocks)
    tiles = w_key.shape[1] // LANES
    rows = queries.shape[0]
    return pl.pallas_call(
        functools.partial(attention_kernel, (NOPE + ROPE) ** (-0.5), len(blocks)),
        out_shape=jax.ShapeDtypeStruct((rows, w_value.shape[1]), jnp.bfloat16),
        in_specs=[HBM] * (len(blocks) + 5),
        out_specs=HBM,
        scratch_shapes=[
            pltpu.VMEM((tiles, keys, 2 * LANES), jnp.bfloat16),
            pltpu.VMEM((keys, w_value.shape[1]), jnp.bfloat16),
            pltpu.VMEM((keys, blocks[0].shape[1]), jnp.bfloat16),
            pltpu.VMEM(queries.shape, queries.dtype),
            pltpu.VMEM(cosine.shape, cosine.dtype),
            pltpu.VMEM(sine.shape, sine.dtype),
            pltpu.VMEM(w_key.shape, w_key.dtype),
            pltpu.VMEM(w_value.shape, w_value.dtype),
            pltpu.VMEM((rows, w_value.shape[1]), jnp.bfloat16),
            pltpu.SemaphoreType.DMA((len(blocks) + 5,)),
        ],
        compiler_params=PARAMS,
        name="attend",
    )(queries, cosine, sine, *blocks, w_key, w_value)


def mix_kernel(*refs):
    heads = refs[0:4]
    w_refs = refs[4:8]
    resid_refs = refs[8:12]
    out_hbm, hid_ref, h_scr, w_scr, in_scr, sems = refs[12:]
    _, p, y, c = coordinates()
    turned = (p + c) % PAIR
    rows, share = heads[0].shape
    depth = w_refs[0].shape[0]
    width = resid_refs[0].shape[1]
    copies = []
    for j, (dy, k) in enumerate(ROUNDS):
        columns = pl.ds(pl.multiple_of(round_block(dy, k, p, y) * width, width), width)
        copies.append(
            pltpu.make_async_copy(resid_refs[j], in_scr.at[:, columns], sems.at[0, j])
        )
        columns = pl.ds(j * share, share)
        copies.append(pltpu.make_async_copy(heads[j], h_scr.at[:, columns], sems.at[1, j]))
        slot = j + turned * (1 - 2 * (j % PAIR))
        span = pl.ds(pl.multiple_of(slot * depth, depth), depth)
        copies.append(pltpu.make_async_copy(w_refs[j], w_scr.at[span], sems.at[2, j]))
    for copy in copies:
        copy.start()
    for copy in copies:
        copy.wait()
    gains = in_scr[rows:, :].astype(jnp.float32)
    gain = gains[0:1] + gains[1:2] + gains[2:3]
    chunk = rows // 4
    outs = []
    for start in range(0, rows, chunk):
        span = slice(start, start + chunk)
        mixed = jnp.dot(h_scr[span, :], w_scr[...], preferred_element_type=jnp.float32)
        mixed = mixed + DEEP_ALPHA * in_scr[span, :].astype(jnp.float32)
        mean = jnp.mean(mixed, axis=1, keepdims=True)
        variance = jnp.mean(mixed * mixed, axis=1, keepdims=True) - mean * mean
        hid_ref[span, :] = ((mixed - mean) * lax.rsqrt(variance + NORM_EPSILON) * gain).astype(
            jnp.bfloat16
        )
        part = pl.ds(start, chunk)
        copy = pltpu.make_async_copy(hid_ref.at[part], out_hbm.at[part], sems.at[3, len(outs)])
        copy.start()
        outs.append(copy)
    for copy in outs:
        copy.wait()


def mix(heads, w_pieces, resid_pieces):
    rows, share = heads[0].shape
    depth, width_total = w_pieces[0].shape
    return pl.pallas_call(
        mix_kernel,
        out_shape=jax.ShapeDtypeStruct((rows, width_total), jnp.bfloat16),
        in_specs=[HBM] * 12,
        out_specs=HBM,
        scratch_shapes=[
            pltpu.VMEM((rows, width_total), jnp.bfloat16),
            pltpu.VMEM((rows, 4 * share), jnp.bfloat16),
            pltpu.VMEM((4 * depth, width_total), jnp.bfloat16),
            pltpu.VMEM((resid_pieces[0].shape[0], width_total), jnp.bfloat16),
            pltpu.SemaphoreType.DMA((4, 4)),
        ],
        compiler_params=PARAMS,
        name="mix",
    )(*heads, *w_pieces, *resid_pieces)


def homes(r):
    high = r // PAIR
    low = r % PAIR
    return ((high, low), (high, other(low)), (other(high), low), (other(high), other(low)))


def up_kernel(own_ref, got_ref, *refs):
    n_pieces = RING * PAIR
    pieces = refs[:n_pieces]
    out_hbm, out_ref, h_scr, w_scr, sems = refs[n_pieces:]
    r, p, _, _ = coordinates()
    depth = pieces[0].shape[0]
    units = out_ref.shape[1]
    rows = own_ref.shape[0]
    hidden = []
    weights = []
    for kind, part in enumerate((p, other(p))):
        for at, (row, column) in enumerate(homes(r)):
            slot = kind * RING + at
            span = pl.ds(slot * depth, depth)
            weights.append(pltpu.make_async_copy(pieces[slot], w_scr.at[span], sems.at[2, slot]))
            block = row * PAIR * PAIR + part * PAIR + column
            columns = pl.ds(pl.multiple_of(block * depth, depth), depth)
            for side, ref in enumerate((own_ref, got_ref)):
                hidden.append(
                    pltpu.make_async_copy(
                        ref.at[:, columns],
                        h_scr.at[pl.ds(side * rows, rows), span],
                        sems.at[side, slot],
                    )
                )
    for copy in hidden + weights:
        copy.start()
    for copy in hidden + weights:
        copy.wait()
    both = jnp.dot(h_scr[...], w_scr[...], preferred_element_type=jnp.float32)
    gate = both[:, :units]
    out_ref[...] = (gate / (1.0 + jnp.exp(-gate)) * both[:, units:]).astype(jnp.bfloat16)
    done = pltpu.make_async_copy(out_ref, out_hbm, sems.at[0, 0])
    done.start()
    done.wait()


def feed_up(own, got, pieces):
    rows, width_total = own.shape
    units = pieces[0].shape[1] // 2
    return pl.pallas_call(
        up_kernel,
        out_shape=jax.ShapeDtypeStruct((PAIR * rows, units), jnp.bfloat16),
        in_specs=[HBM] * (2 + len(pieces)),
        out_specs=HBM,
        scratch_shapes=[
            pltpu.VMEM((PAIR * rows, units), jnp.bfloat16),
            pltpu.VMEM((PAIR * rows, width_total), jnp.bfloat16),
            pltpu.VMEM((width_total, 2 * units), jnp.bfloat16),
            pltpu.SemaphoreType.DMA((3, len(pieces))),
        ],
        compiler_params=PARAMS,
        name="feed_up",
    )(own, got, *pieces)


def down_kernel(own_ref, got_ref, *refs):
    downs = refs[:8]
    outs = refs[8:12]
    o_scr, a_scr, d_scr, sems = refs[12:]
    r, p, y, c = coordinates()
    depth = downs[0].shape[1]
    rows = a_scr.shape[1]
    units = own_ref.shape[1]
    copies = []
    for side in range(2):
        group = c if side == 0 else other(c)
        mine = pl.ds(side * rows, rows)
        theirs = pl.ds((1 - side) * rows, rows)
        copies.append(
            pltpu.make_async_copy(
                own_ref.at[mine], a_scr.at[group, :, pl.ds(0, units)], sems.at[side]
            )
        )
        copies.append(
            pltpu.make_async_copy(
                got_ref.at[theirs], a_scr.at[group, :, pl.ds(units, units)], sems.at[2 + side]
            )
        )
    for at, (row, column) in enumerate(homes(r)):
        columns = pl.ds(pl.multiple_of(column * depth, depth), depth)
        for side in range(2):
            slot = side * 4 + at
            span = pl.ds(side * units, units)
            copies.append(
                pltpu.make_async_copy(
                    downs[slot], d_scr.at[row, span, columns], sems.at[4 + slot]
                )
            )
    for copy in copies:
        copy.start()
    for copy in copies:
        copy.wait()
    stores = []
    for j, (dy, dp) in enumerate(ROUNDS):
        group = other(p) if dp else p
        row = other(y) if dy else y
        o_scr[j] = jnp.dot(a_scr[group], d_scr[row], preferred_element_type=jnp.float32).astype(
            jnp.bfloat16
        )
        copy = pltpu.make_async_copy(o_scr.at[j], outs[j], sems.at[12 + j])
        copy.start()
        stores.append(copy)
    for copy in stores:
        copy.wait()


def feed_down(own, got, downs):
    rows = own.shape[0] // PAIR
    units = PAIR * downs[0].shape[0]
    depth = downs[0].shape[1]
    block = jax.ShapeDtypeStruct((rows, PAIR * depth), jnp.bfloat16)
    return pl.pallas_call(
        down_kernel,
        out_shape=(block,) * 4,
        in_specs=[HBM] * 10,
        out_specs=(HBM,) * 4,
        scratch_shapes=[
            pltpu.VMEM((4, rows, PAIR * depth), jnp.bfloat16),
            pltpu.VMEM((PAIR, rows, units), jnp.bfloat16),
            pltpu.VMEM((PAIR, units, PAIR * depth), jnp.bfloat16),
            pltpu.SemaphoreType.DMA((16,)),
        ],
        compiler_params=PARAMS,
        name="feed_down",
    )(own, got, *downs)


def sum_kernel(own_ref, got_ref, *refs):
    terms = refs[:4]
    pre_ref, stat_ref, t_scr, h_scr, sems = refs[4:]
    _, p, y, c = coordinates()
    rows, width = pre_ref.shape
    copies = []
    for j in range(4):
        copy = pltpu.make_async_copy(terms[j], t_scr.at[j], sems.at[j])
        copy.start()
        copies.append(copy)
    columns = pl.ds(pl.multiple_of((y * PAIR + c) * width, width), width)
    for side, ref in enumerate((own_ref, got_ref)):
        copy = pltpu.make_async_copy(ref.at[:, columns], h_scr.at[side], sems.at[4 + side])
        copy.start()
        copies.append(copy)
    for copy in copies:
        copy.wait()
    total = jnp.zeros((rows, width), jnp.float32)
    for j in range(4):
        total = total + t_scr[j].astype(jnp.float32)
    skip = h_scr[(p + c) % PAIR].astype(jnp.float32)
    pre = DEEP_ALPHA * skip + HALF_STEP * total
    pre_ref[...] = pre
    lane = lax.broadcasted_iota(jnp.int32, (rows, LANES), 1)
    sums = jnp.sum(pre, axis=1, keepdims=True)
    squares = jnp.sum(pre * pre, axis=1, keepdims=True)
    table = jnp.where(lane == 0, sums, jnp.where(lane == 1, squares, 0.0))
    stat_ref[...] = jnp.transpose(table)[: stat_ref.shape[0], :]


def add_up(own, got, terms):
    rows, width = terms[0].shape
    return pl.pallas_call(
        sum_kernel,
        out_shape=(
            jax.ShapeDtypeStruct((rows, width), jnp.float32),
            jax.ShapeDtypeStruct((8, rows), jnp.float32),
        ),
        in_specs=[HBM] * 6,
        out_specs=(VMEM,) * 2,
        scratch_shapes=[
            pltpu.VMEM((4, rows, width), jnp.bfloat16),
            pltpu.VMEM((2, rows, width), jnp.bfloat16),
            pltpu.SemaphoreType.DMA((6,)),
        ],
        compiler_params=PARAMS,
        name="add_up",
    )(own, got, *terms)


def norm_kernel(width_total, pre_ref, a_ref, b_ref, c_ref, d_ref, gain_ref, out_ref):
    stats = a_ref[...] + b_ref[...] + c_ref[...] + d_ref[...]
    tall = jnp.concatenate(
        [stats, jnp.zeros((LANES - stats.shape[0], stats.shape[1]), jnp.float32)], axis=0
    )
    table = jnp.transpose(tall)
    mean = table[:, 0:1] / width_total
    variance = table[:, 1:2] / width_total - mean * mean
    out_ref[...] = (
        (pre_ref[...] - mean) * lax.rsqrt(variance + NORM_EPSILON) * gain_ref[...]
    ).astype(jnp.bfloat16)


def finish(pre, stats, gain):
    return pl.pallas_call(
        functools.partial(norm_kernel, pre.shape[1] * PAIR * PAIR),
        out_shape=jax.ShapeDtypeStruct(pre.shape, jnp.bfloat16),
        in_specs=[VMEM] * 6,
        out_specs=VMEM,
        compiler_params=PARAMS,
        name="finish",
    )(pre, *stats, gain.reshape(1, -1))


def three_terms(gain):
    first = lax.reduce_precision(gain, 8, 7)
    left = gain - first
    second = lax.reduce_precision(left, 8, 7)
    third = left - second
    return jnp.stack([first, second, third]).astype(jnp.bfloat16)


def planned(*arrays):
    return planned_steps(*arrays)


def planned_steps(
    queries,
    latents,
    rope_key,
    w_key,
    w_value,
    w_out,
    resid,
    gain_mix,
    w_gate,
    w_up,
    w_down,
    gain_out,
):
    _, p, _, c = coordinates()
    local_rows = queries.shape[0]
    positions = lax.axis_index("sp") * local_rows + jnp.arange(local_rows, dtype=jnp.int32)
    cosine, sine = rotary_tables(positions, ROPE, GRID_W)
    key_rot = rotate(rope_key, cosine, sine)

    half = local_rows // PAIR
    wide = jnp.concatenate(
        [latents, key_rot, jnp.zeros((local_rows, LANES - ROPE), jnp.bfloat16)], axis=1
    )
    piece = lax.dynamic_slice_in_dim(wide, c * half, half, 0)
    near = flip(piece, dp=1)
    far = flip(piece, dr=2, dp=1)
    cut = half // 2
    across_low = flip(far[:cut], dp=1)
    across_high = flip(near[cut:], dr=2, dp=1)
    crossed = flip(piece, dr=1)
    first = jnp.concatenate([near, far], axis=0)
    first = [piece, first, crossed, flip(first, dr=1)]
    last = jnp.concatenate([across_low, across_high], axis=0)
    last = [last, flip(last, dr=1)]
    first = jnp.concatenate(first, axis=0)
    first = [first, partner(first)]
    last = jnp.concatenate(last, axis=0)
    last = [last, partner(last)]
    blocks = first + last

    width = w_gate.shape[1] // PAIR
    keep, give = p * width, other(p) * width
    chunks = {
        "a": jnp.concatenate(
            [lax.dynamic_slice_in_dim(w, keep, width, 1) for w in (w_gate, w_up)], axis=1
        )
    }
    chunks["b"] = flip(
        jnp.concatenate(
            [lax.dynamic_slice_in_dim(w, give, width, 1) for w in (w_gate, w_up)], axis=1
        ),
        dp=1,
    )
    down_own = lax.dynamic_slice_in_dim(w_down, keep, width, 0)
    down_got = flip(lax.dynamic_slice_in_dim(w_down, give, width, 0), dp=1)
    heads_own = attend(queries, cosine, sine, blocks, w_key, w_value)
    down_got, heads_own = lax.optimization_barrier((down_got, heads_own))
    down_mine = jnp.where(p == c, down_own, down_got)
    down_theirs = partner(jnp.where(p == c, down_got, down_own))
    chunks["e"] = down_mine
    chunks["f"] = down_theirs

    gathered = {}
    for name, shard in chunks.items():
        w_near = flip(shard, dr=1)
        w_far = flip(shard, dr=2)
        w_across = flip(w_far, dr=1)
        gathered[name] = [shard, w_near, w_far, w_across]

    gains = jnp.pad(three_terms(gain_mix), ((0, 13), (0, 0)))
    resid_own = jnp.concatenate([resid, gains], axis=0)
    resid_pieces = []
    for dy, k in ROUNDS:
        resid_pieces.append(spread(resid_own, dy, k))
    out_other = flip(w_out, dy=1)
    w_partner = partner(w_out)
    out_last = partner(out_other)
    w_pieces = [w_out, w_partner, out_other, out_last]
    heads = []
    for dy, k in ROUNDS:
        heads.append(spread(heads_own, dy, k))
    hidden = mix(heads, w_pieces, resid_pieces)
    got = partner(hidden)
    act = feed_up(hidden, got, gathered["a"] + gathered["b"])
    act_got = partner(act)
    terms = list(feed_down(act, act_got, gathered["e"] + gathered["f"]))
    for at, (dy, dp) in enumerate(ROUNDS):
        if dy or dp:
            terms[at] = flip(terms[at], dp=dp, dy=dy)
    pre, stats = add_up(hidden, got, terms)
    stat_y = flip(stats, dy=1)
    stat_yc = flip(stats, dy=1, dc=1)
    stat_c = partner(stats)
    return finish(pre, [stats, stat_c, stat_y, stat_yc], gain_out)


def solution(mesh):
    placed = (
        P("sp", "tp"),
        P("sp", None),
        P("sp", None),
        P(None, "tp"),
        P(None, "tp"),
        P("tp", None),
        P("sp", "tp"),
        P("tp"),
        P("sp", "tp"),
        P("sp", "tp"),
        P("tp", "sp"),
        P("tp"),
    )
    body = planned if fits_plan(mesh) else local
    return jax.shard_map(
        body, mesh=mesh, in_specs=placed, out_specs=P("sp", "tp"), check_vma=False
    )
```
